32 devices in a mesh: ep: 32 (over z, y, x, core).
Axes of the slice: x: 2, y: 2, z: 4, core: 2. Of those that a mesh axis runs over, the one named last changes fastest.
Arguments:
- residual_in: bfloat16 [256, 2048], P('ep'), may hold values from -6 to 6
- gain_mix_pre: float32 [2048], replicated, may hold values from 0.1 to 1.9
- w_query: bfloat16 [2048, 2048], P(None, 'ep'), may hold values from -0.125 to 0.125
- w_key: bfloat16 [2048, 2048], P(None, 'ep'), may hold values from -0.125 to 0.125
- w_value: bfloat16 [2048, 2048], P(None, 'ep'), may hold values from -0.125 to 0.125
- w_outgate: bfloat16 [2048, 2048], P(None, 'ep'), may hold values from -0.125 to 0.125
- w_decay: bfloat16 [2048, 16], replicated, may hold values from -0.125 to 0.125
- w_beta: bfloat16 [2048, 16], replicated, may hold values from -0.125 to 0.125
- decay_scale: float32 [16], replicated, may hold values from 1 to 16
- decay_bias: float32 [16], replicated, may hold values from -5 to -1
- head_gain: float32 [128], replicated, may hold values from 0.1 to 1.9
- w_out: bfloat16 [2048, 2048], replicated, may hold values from -0.125 to 0.125
- gain_mix_post: float32 [2048], replicated, may hold values from 0.1 to 1.9
- state_cache: bfloat16 [256, 16, 128, 128], P('ep'), may hold values from -2.390625 to 2.390625
- gain_ffn_pre: float32 [2048], replicated, may hold values from 0.1 to 1.9
- routes: int32 [256, 4], P('ep'), may hold values from 0 to 7, all different within a row; in each aligned block of 8 rows (0 to 7, 8 to 15, ...) at most 8 rows name the same one
- route_logits: float32 [256, 4], P('ep'), may hold values from -6 to 6
- w_gate: bfloat16 [2048, 16384], P(None, 'ep'), may hold values from -0.375 to 0.375
- w_up: bfloat16 [2048, 16384], P(None, 'ep'), may hold values from -0.375 to 0.375
- w_down: bfloat16 [16384, 2048], P('ep'), may hold values from -0.125 to 0.125
- gain_ffn_post: float32 [2048], replicated, may hold values from 0.1 to 1.9
Outputs:
- result: bfloat16 [256, 2048], P('ep')
- new_state: bfloat16 [256, 16, 128, 128], P('ep')
The draws below stay inside these ranges and needn't reach their ends.
Inputs may be any that keep to these rules, and one draw needn't show every extreme that they name: `routes`: each row names 4 different experts. In the rows of one device (aligned blocks of 8 rows) no expert is named more than 8 times, and in some block one expert is named exactly 8 times.
All inputs are finite; a program needn't handle non-finite values.
Results may differ from the reference program's by a relative error of at most 0.014.
Values may be sent and summed in bfloat16 or wider, within the bound.
A program may use at most 128 MiB of HBM per device.

```python
import math
import jax
import jax.numpy as jnp
import numpy as np
from jax import lax

D = 2048
H = 16
HD = 128
FF = 2048
PIECES = 4
TOPK = 4
SEQ_DEV = 8
TOKENS = 256
EXPERTS = 8
CAP = 8
N_EP = 32


def level_of(own_key, shape, shards, low, top_value):
    def one(position, blocks):
        steps = jax.random.uniform(jax.random.fold_in(jax.random.fold_in(own_key, 6), position), (blocks,), jnp.float32, low / len(shards), top_value / len(shards))
        return jnp.repeat(jnp.exp(steps), shape[position] // blocks).reshape((-1,) + (1,) * (len(shape) - position - 1))

    gain = one(*shards[0])
    for cut in shards[1:]:
        gain = gain * one(*cut)
    return gain


def deal_out(stream_key, own, number, rows, count, top, limit, lean):
    ranking = jax.random.permutation(stream_key, count)
    heavy_load, common = shares(count, rows * top, limit, lean, True), shares(count, rows * top, limit, lean, False)
    places = jnp.arange(count)

    def named(sizes, rotation):
        used = int((sizes > 0).sum())
        fixed = max(1, used // 4)
        moved = fixed + (places - fixed + rotation * (used - fixed)) % max(1, count - fixed)
        return jnp.zeros((count,), jnp.int32).at[ranking[jnp.where(places < fixed, places, moved)]].set(jnp.asarray(sizes, jnp.int32))

    sizes = jnp.where(number % 4 == 0, named(heavy_load, number // 4), named(common, number - number // 4 - 1))
    mixed = jax.random.permutation(jax.random.fold_in(own, 3), count)
    source_of, receiver = mixed[0:count // 2 * 2:2], mixed[1:count // 2 * 2:2]
    room = jnp.minimum(sizes[source_of] - 1, limit - sizes[receiver]) // 2
    room = jnp.where((source_of == ranking[0]) | (receiver == ranking[0]) | (sizes[receiver] == 0), 0, jnp.maximum(room, 0))
    moved = jax.random.randint(jax.random.fold_in(own, 4), (count // 2,), 0, 1 << 20) % (room + 1)
    sizes = sizes.at[source_of].add(-moved).at[receiver].add(moved)
    members = jnp.searchsorted(jnp.cumsum(sizes), jnp.arange(rows * top), side="right").astype(jnp.int32)
    table = members.reshape(top, rows).T
    table = table[jax.random.permutation(jax.random.fold_in(own, 1), rows)]
    rotation = jax.random.randint(jax.random.fold_in(own, 2), (rows, 1), 0, top)
    return jnp.take_along_axis(table, (jnp.arange(top)[None, :] + rotation) % top, axis=1)


def shares(number_of, total, bound, slope, full):
    loads = [(1 << 20) // math.isqrt(standing ** slope) + 1 for standing in range(1, number_of + 1)]
    largest = bound if full else min(bound, max(-(-total // number_of), total * loads[0] // sum(loads)))
    least = 1 if total - largest >= number_of - 1 else 0
    holding, rest = [largest] + [least] * (number_of - 1), total - largest - least * (number_of - 1)
    while rest > 0:
        free = [i for i in range(1, number_of) if holding[i] < largest] or [i for i in range(1, number_of) if holding[i] < bound]
        mass, remaining = sum([loads[i] for i in free]), rest
        for i in free:
            more = min(bound - holding[i], max(1, remaining * loads[i] // mass), rest)
            holding[i] = holding[i] + more
            rest = rest - more
    return np.array(holding)


def noise(key, shape, scale, limit, pieces=(), held_as=jnp.bfloat16):
    values = scale * jax.random.normal(key, shape, jnp.float32)
    if pieces:
        values = values * level_of(key, shape, pieces, -0.22, 0.18)
    return jnp.clip(values, -limit, limit).astype(held_as)


def setup_inputs(seed: int = 0) -> dict:
    key_of = jax.random.split(jax.random.key(seed), 22)
    residual_in = noise(key_of[0], (TOKENS, D), 1.0, 6.0, ((0, 32),))
    gain_mix_pre = jnp.clip(1.0 + 0.18 * jax.random.normal(key_of[1], (D,), jnp.float32), 0.1, 1.9)
    w_query = noise(key_of[2], (D, H * HD), D ** -0.5, 0.125, ((1, 32),))
    w_key = noise(key_of[3], (D, H * HD), D ** -0.5, 0.125, ((1, 32),))
    w_value = noise(key_of[4], (D, H * HD), D ** -0.5, 0.125, ((1, 32),))
    w_outgate = noise(key_of[5], (D, H * HD), D ** -0.5, 0.125, ((1, 32),))
    w_decay = noise(key_of[6], (D, H), D ** -0.5, 0.125)
    w_beta = noise(key_of[7], (D, H), D ** -0.5, 0.125)
    decay_scale = jnp.clip(jnp.exp(jax.random.uniform(key_of[8], (H,), jnp.float32, math.log(1.0), math.log(16.0))), 1.0, 16.0)
    decay_bias = jnp.clip(jax.random.uniform(key_of[9], (H,), jnp.float32, -5.0, -1.0), -5.0, -1.0)
    head_gain = jnp.clip(1.0 + 0.18 * jax.random.normal(key_of[10], (HD,), jnp.float32), 0.1, 1.9)
    w_out = noise(key_of[11], (H * HD, D), (H * HD) ** -0.5, 0.125)
    gain_mix_post = jnp.clip(1.0 + 0.18 * jax.random.normal(key_of[12], (D,), jnp.float32), 0.1, 1.9)
    state_cache = noise(key_of[13], (TOKENS, H, HD, HD), 0.3, 2.390625, ((0, 32),))
    gain_ffn_pre = jnp.clip(1.0 + 0.18 * jax.random.normal(key_of[14], (D,), jnp.float32), 0.1, 1.9)
    routes_keys = jax.random.split(jax.random.fold_in(key_of[15], 1), TOKENS // SEQ_DEV)
    routes_turns = jax.random.permutation(jax.random.fold_in(key_of[15], 3), TOKENS // SEQ_DEV)
    routes = jax.vmap(lambda own, number: deal_out(jax.random.fold_in(key_of[15], 2), own, number, SEQ_DEV, EXPERTS, TOPK, CAP, 1))(routes_keys, routes_turns).reshape((TOKENS, TOPK))
    route_logits = noise(key_of[16], (TOKENS, TOPK), 1.0, 6.0, ((0, 32),), jnp.float32)
    w_gate = noise(key_of[17], (D, EXPERTS * FF), (D // 9) ** -0.5, 0.375, ((1, 32),))
    w_up = noise(key_of[18], (D, EXPERTS * FF), (D // 9) ** -0.5, 0.375, ((1, 32),))
    w_down = noise(key_of[19], (EXPERTS * FF, D), FF ** -0.5, 0.125, ((0, 32),))
    gain_ffn_post = jnp.clip(1.0 + 0.18 * jax.random.normal(key_of[20], (D,), jnp.float32), 0.1, 1.9)
    return dict(residual_in=residual_in, gain_mix_pre=gain_mix_pre, w_query=w_query, w_key=w_key, w_value=w_value, w_outgate=w_outgate, w_decay=w_decay, w_beta=w_beta, decay_scale=decay_scale, decay_bias=decay_bias, head_gain=head_gain, w_out=w_out, gain_mix_post=gain_mix_post, state_cache=state_cache, gain_ffn_pre=gain_ffn_pre, routes=routes, route_logits=route_logits, w_gate=w_gate, w_up=w_up, w_down=w_down, gain_ffn_post=gain_ffn_post)


EPS = 1e-06
LIMIT = 7.0
ALPHA = 1.702

def rms_scale(values):
    return values * lax.rsqrt(lax.optimization_barrier(jnp.mean(values * values, axis=-1, keepdims=True)) + EPS)

def clamped_unit(gate, upper):
    glu = jnp.minimum(gate, LIMIT)
    linear = jnp.clip(upper, -LIMIT, LIMIT)
    return glu * jax.nn.sigmoid(ALPHA * glu) * (linear + 1.0)

def dispatch_table(routes, experts, capacity):
    count, topk = routes.shape
    hits = (routes[:, :, None] == jnp.arange(experts, dtype=jnp.int32)).astype(jnp.int32)
    flat = hits.reshape(count * topk, experts)
    before = jnp.cumsum(flat, axis=0) - flat
    slots = lax.optimization_barrier(jnp.sum(before * flat, axis=1)).reshape(count, topk)
    target = routes * capacity + slots
    return (target[:, :, None] == jnp.arange(experts * capacity, dtype=jnp.int32)).astype(jnp.float32)

def delta_step(q_raw, k_raw, v_raw, z_raw, decay_in, beta_in, state, decay_scale, decay_bias, head_gain):
    count = q_raw.shape[0]
    query = jax.nn.silu(q_raw.astype(jnp.float32)).reshape(count, H, HD)
    query = query * lax.rsqrt(lax.optimization_barrier(jnp.sum(query * query, axis=-1, keepdims=True)) + EPS) * HD ** (-0.5)
    keys = jax.nn.silu(k_raw.astype(jnp.float32)).reshape(count, H, HD)
    keys = keys * lax.rsqrt(lax.optimization_barrier(jnp.sum(keys * keys, axis=-1, keepdims=True)) + EPS)
    values = jax.nn.silu(v_raw.astype(jnp.float32)).reshape(count, H, HD)
    decay = -decay_scale * jax.nn.softplus(decay_in + decay_bias)
    beta = jax.nn.sigmoid(beta_in)
    held = state.astype(jnp.float32) * jnp.exp(decay)[:, :, None, None]
    guess = jnp.einsum('rhk,rhkv->rhv', keys, held)
    held = held + jnp.einsum('rhk,rhv->rhkv', keys, beta[:, :, None] * (values - guess))
    output = jnp.einsum('rhk,rhkv->rhv', query, held)
    output = rms_scale(output) * head_gain
    gated = output.reshape(count, H * HD) * jax.nn.silu(z_raw.astype(jnp.float32))
    return (gated.astype(jnp.bfloat16), held.astype(jnp.bfloat16))

def reference(residual_in, gain_mix_pre, w_query, w_key, w_value, w_outgate, w_decay, w_beta, decay_scale, decay_bias, head_gain, w_out, gain_mix_post, state_cache, gain_ffn_pre, routes, route_logits, w_gate, w_up, w_down, gain_ffn_post):
    x_first = residual_in.astype(jnp.float32)
    normed = (rms_scale(x_first) * gain_mix_pre).astype(jnp.bfloat16)

    def project(weight):
        return jnp.dot(normed, weight, preferred_element_type=jnp.float32).astype(jnp.bfloat16)
    q_raw, k_raw, v_raw, z_raw = (project(w_query), project(w_key), project(w_value), project(w_outgate))
    decay_in = jnp.dot(normed, w_decay, preferred_element_type=jnp.float32)
    beta_in = jnp.dot(normed, w_beta, preferred_element_type=jnp.float32)

    def blocks(array):
        return array.reshape((N_EP, SEQ_DEV) + array.shape[1:])

    def block_step(items):
        return delta_step(*items, decay_scale, decay_bias, head_gain)
    mixed, new_state = lax.map(block_step, tuple((blocks(a) for a in (q_raw, k_raw, v_raw, z_raw, decay_in, beta_in, state_cache))))
    mixed = mixed.reshape(TOKENS, H * HD)
    new_state = new_state.reshape(TOKENS, H, HD, HD)
    branch = jnp.dot(mixed, w_out, preferred_element_type=jnp.float32)
    x_second = x_first + rms_scale(branch) * gain_mix_post
    normed_two = (rms_scale(x_second) * gain_ffn_pre).astype(jnp.bfloat16)
    table = jax.vmap(lambda r: dispatch_table(r, EXPERTS, CAP))(routes.reshape(N_EP, SEQ_DEV, TOPK))
    picks = lax.optimization_barrier(jnp.sum(table, axis=2))
    sent = jnp.einsum('nse,nsd->ned', picks, normed_two.reshape(N_EP, SEQ_DEV, D).astype(jnp.float32), precision=lax.Precision.HIGHEST).astype(jnp.bfloat16)
    sent = sent.reshape(N_EP, EXPERTS, CAP, D).transpose(1, 0, 2, 3).reshape(EXPERTS, N_EP * CAP, D)
    width = FF // PIECES

    def expert(items):
        rows_in, index = items
        total = jnp.zeros((N_EP * CAP, D), jnp.float32)
        for part in range(PIECES):
            start = (index * FF + part * width).astype(jnp.int32)
            gate_cols = lax.dynamic_slice_in_dim(w_gate, start, width, 1)
            up_cols = lax.dynamic_slice_in_dim(w_up, start, width, 1)
            down_rows = lax.dynamic_slice_in_dim(w_down, start, width, 0)
            hidden = clamped_unit(jnp.dot(rows_in, gate_cols, preferred_element_type=jnp.float32), jnp.dot(rows_in, up_cols, preferred_element_type=jnp.float32)).astype(jnp.bfloat16)
            piece_out = jnp.dot(hidden, down_rows, preferred_element_type=jnp.float32).astype(jnp.bfloat16)
            piece_out = lax.optimization_barrier(piece_out)
            total = total + piece_out.astype(jnp.float32)
        return total
    outputs = lax.map(expert, (sent, jnp.arange(EXPERTS, dtype=jnp.int32)))
    outputs = outputs.reshape(EXPERTS, N_EP, CAP, D).transpose(1, 0, 2, 3).reshape(N_EP, EXPERTS * CAP, D)
    raised = jnp.exp(route_logits)
    weights = raised / lax.optimization_barrier(jnp.sum(raised, axis=-1, keepdims=True))
    mix_table = jnp.einsum('nske,nsk->nse', table, weights.reshape(N_EP, SEQ_DEV, TOPK))
    moe = jnp.einsum('nse,ned->nsd', mix_table, outputs, precision=lax.Precision.HIGHEST).reshape(TOKENS, D)
    result = (x_second + rms_scale(moe) * gain_ffn_post).astype(jnp.bfloat16)
    return (result, new_state)
```

```python
import functools
import types

import jax
import jax.numpy as jnp
from jax import lax
from jax.experimental import pallas as pl
from jax.experimental.pallas import tpu as pltpu
from jax.sharding import PartitionSpec as P

H = 16
HD = 128
PIECES = 4
TOPK = 4
LANES = 128
HALF = LANES // 2
VMEM_LIMIT = 58 * 1000 * 1000
MESH = pl.DeviceIdType.MESH

EPS = 1e-06
LIMIT = 7.0
ALPHA = 1.702


def rms_scale(values):
    return values * lax.rsqrt(jnp.mean(values * values, axis=-1, keepdims=True) + EPS)


def clamped_unit(gate, upper):
    glu = jnp.minimum(gate, LIMIT)
    linear = jnp.clip(upper, -LIMIT, LIMIT)
    return glu * jax.nn.sigmoid(ALPHA * glu) * (linear + 1.0)


def flipped(value, distance):
    bit = 1
    while bit <= distance:
        if distance & bit:
            value = value + bit - 2 * bit * (lax.rem(value // bit, 2))
        bit *= 2
    return value


class Place:
    def __init__(self, devices):
        self.layers = devices // 8
        self.me = lax.axis_index("ep")
        self.core = lax.rem(self.me, 2)
        self.x = lax.rem(self.me // 2, 2)
        self.y = lax.rem(self.me // 4, 2)
        self.z = self.me // 8
        self.chip = self.me // 2
        self.partner = flipped(self.me, 1)

    def at(self, distance=0, y=0, x=0):
        z = flipped(self.z, distance)
        return z * 8 + flipped(self.y, y) * 4 + flipped(self.x, x) * 2 + self.core

    def slot(self, distance=0, y=0, x=0):
        return distance * 4 + flipped(self.y, y) * 2 + flipped(self.x, x)


def greet(partners):
    barrier = pltpu.get_barrier_semaphore()
    for partner in partners:
        pl.semaphore_signal(barrier, inc=1, device_id=(partner,), device_id_type=MESH)
    return lambda: pl.semaphore_wait(barrier, len(partners))


def load_all(pairs, sems):
    loads = [
        pltpu.make_async_copy(source, target, sems.at[i])
        for i, (source, target) in enumerate(pairs)
    ]
    for load in loads:
        load.start()
    return loads


def remote(source, target, send_sem, recv_sem, device):
    return pltpu.make_async_remote_copy(
        src_ref=source,
        dst_ref=target,
        send_sem=send_sem,
        recv_sem=recv_sem,
        device_id=(device,),
        device_id_type=MESH,
    )


def gather_sends(devices):
    return 4 * (devices // 8) - 1


PLANE = ((1, 1), (0, 1), (1, 0))


class Gather:
    def __init__(self, place, buf, send_sems, recv_sems):
        self.place, self.buf = place, buf
        self.send_sems, self.recv_sems = send_sems, recv_sems
        self.started = []

    def push(self, source, target, device):
        copy = remote(
            self.buf.at[source],
            self.buf.at[target],
            self.send_sems.at[len(self.started)],
            self.recv_sems.at[target],
            device,
        )
        copy.start()
        self.started.append(copy)

    def arrive(self, slot):
        remote(
            self.buf.at[slot],
            self.buf.at[slot],
            self.send_sems.at[0],
            self.recv_sems.at[slot],
            self.place.partner,
        ).wait_recv()

    def spread(self, distance):
        place = self.place
        slot = place.slot(distance)
        for y, x in PLANE:
            self.push(slot, slot, place.at(y=y, x=x))

    def column(self, distance):
        self.arrive(self.place.slot(distance))
        self.spread(distance)

    def across(self, distance):
        for y, x in reversed(PLANE):
            self.arrive(self.place.slot(distance, y, x))

    def begin(self):
        place = self.place
        for distance in range(1, place.layers):
            self.push(place.slot(), place.slot(distance), place.at(distance))
        self.spread(0)

    def relays(self):
        return [functools.partial(self.column, d) for d in range(1, self.place.layers)]


class Scatter:
    def __init__(self, place, parts, plane, column, sems):
        self.place, self.parts = place, parts
        self.plane, self.column = plane, column
        self.send_sems, self.plane_recv, self.column_recv = sems
        self.started = []
        self.value = None

    def push(self, source, target, recv_sem, device):
        copy = remote(source, target, self.send_sems.at[len(self.started)], recv_sem, device)
        copy.start()
        self.started.append(copy)

    def arrive(self, target, recv_sem):
        remote(target, target, self.send_sems.at[0], recv_sem, self.place.partner).wait_recv()

    def first(self, distance):
        place = self.place
        for i, (y, x) in enumerate(PLANE):
            at = 3 * distance + i
            self.push(
                self.parts.at[place.slot(distance, y, x)],
                self.plane.at[at],
                self.plane_recv.at[at],
                place.at(y=y, x=x),
            )

    def last(self, distance):
        place = self.place
        slot = place.slot(distance)
        value = wide(self.parts[slot])
        for i in reversed(range(3)):
            at = 3 * distance + i
            self.arrive(self.plane.at[at], self.plane_recv.at[at])
            value = value + wide(self.plane[at])
        if distance > 0:
            self.parts[slot] = value.astype(jnp.bfloat16)
            self.push(
                self.parts.at[slot],
                self.column.at[distance],
                self.column_recv.at[distance],
                place.at(distance),
            )
        else:
            self.value = value

    def collect(self, distance):
        self.arrive(self.column.at[distance], self.column_recv.at[distance])
        self.value = self.value + wide(self.column[distance])


def settle(started):
    for copy in started:
        copy.wait_send()


def wide(block):
    return block.astype(jnp.float32)


def dot_t(left, right):
    return lax.dot_general(
        left, right, (((1,), (1,)), ((), ())), preferred_element_type=jnp.float32
    )


def column_of(row):
    size = row.shape[1]
    across = lax.broadcasted_iota(jnp.int32, (size, size), 1)
    down = lax.broadcasted_iota(jnp.int32, (size, size), 0)
    return jnp.sum(
        jnp.where(across == down, jnp.broadcast_to(row, (size, size)), 0.0), axis=1, keepdims=True
    )


def share_rows(routes, logits):
    raised = jnp.exp(logits)
    shares = raised / jnp.sum(raised, axis=0, keepdims=True)
    routes = routes.astype(jnp.float32)
    count = routes.shape[1]
    lane = lax.broadcasted_iota(jnp.int32, (count, LANES), 1)
    expert = lax.rem(lane, HALF).astype(jnp.float32)
    share = jnp.zeros((count, LANES), jnp.float32)
    for j in range(routes.shape[0]):
        share = share + jnp.where(
            expert == column_of(routes[j : j + 1]), column_of(shares[j : j + 1]), 0.0
        )
    high = share.astype(jnp.bfloat16)
    low = (share - wide(high)).astype(jnp.bfloat16)
    return jnp.where(lane < HALF, wide(high), wide(low)).astype(jnp.bfloat16)


def head_rows(joined, head, kind, piece):
    lane = lax.broadcasted_iota(jnp.int32, (joined.shape[1], LANES), 1)
    value = jnp.zeros(lane.shape, jnp.float32)
    group, offset = divmod(kind * piece, LANES)
    for i in range(HD // piece):
        part = joined[head * (HD // piece) + i, :, group * LANES : (group + 1) * LANES]
        part = wide(part)
        shift = (i * piece - offset) % LANES
        if shift:
            part = pltpu.roll(part, shift, 1)
        value = jnp.where((lane >= i * piece) & (lane < (i + 1) * piece), part, value)
    return value


def all_heads(joined, heads, kind, piece):
    if piece == HD:
        return wide(joined[:, :, kind * HD : (kind + 1) * HD])
    return jnp.stack([head_rows(joined, head, kind, piece) for head in range(heads)])


def inverse_norm(values):
    return lax.rsqrt(jnp.sum(values * values, axis=-1, keepdims=True) + EPS)


INPUTS = (
    "x",
    "gain",
    "routes",
    "logits",
    "w_decay",
    "w_beta",
    "scale",
    "bias",
    "head_gain",
    "gain_mix",
    "gain_pre",
    "gain_post",
    "query",
    "key",
    "value",
    "outgate",
    "state",
    "w_out",
    "gate",
    "up",
    "down",
)
SMALL = INPUTS[:12]


def decode_kernel(devices, names, *refs):
    r = types.SimpleNamespace(**dict(zip(names, refs)))
    place = Place(devices)
    layers, pairs = place.layers, devices // 2
    core, other = place.core, 1 - place.core
    count, width = r.x.shape
    heads = r.keys.shape[0]
    piece = 2 * r.query_hbm.shape[0]
    hidden_units = r.gate_hbm.shape[1]
    half = max(1, layers // 2)
    chunks = [c for c in (range(0, half), range(half, layers)) if len(c)]

    ready = greet(
        [place.at(distance) for distance in range(1, layers)]
        + [place.at(y=y, x=x) for y, x in PLANE]
        + [place.partner]
    )
    loads = load_all(
        [(getattr(r, name + "_hbm"), getattr(r, name)) for name in SMALL], r.small_sems
    )
    projections = (r.query_hbm, r.key_hbm, r.value_hbm, r.outgate_hbm)
    experts = ((r.gate_hbm, r.gate), (r.up_hbm, r.up), (r.down_hbm, r.down))
    weight_loads = load_all(
        [(ref, r.weights.at[i, core]) for i, ref in enumerate(projections)], r.weight_sems
    )
    loads[0].wait()
    loads[1].wait()
    normed = (rms_scale(wide(r.x[...])) * r.gain[...]).astype(jnp.bfloat16)
    gather = Gather(place, r.rows_one, r.one_send, r.one_recv)
    r.rows_one[place.slot()] = normed
    ready()
    gather.begin()
    swaps = [
        remote(
            ref, r.weights.at[i, core], r.swap_send.at[i], r.swap_recv.at[i], place.partner
        )
        for i, ref in enumerate(projections)
    ]
    for swap in swaps:
        swap.start()
    late_loads = load_all(
        [(r.state_hbm, r.state), (r.w_out_hbm, r.w_out)]
        + [(ref, into.at[core]) for ref, into in experts],
        r.late_sems,
    )
    for step in gather.relays():
        step()
    sent = []
    for number, chunk in enumerate(chunks):
        for distance in chunk:
            gather.across(distance)
        if not number:
            for load in weight_loads:
                load.wait()
            for i, ref in enumerate(projections):
                remote(
                    ref,
                    r.weights.at[i, other],
                    r.swap_send.at[i],
                    r.swap_recv.at[i],
                    place.partner,
                ).wait_recv()
        a, b = 4 * chunk[0], 4 * (chunk[-1] + 1)
        rows = r.rows_one[a:b].reshape((b - a) * count, width)
        weights = r.weights[...].reshape(4 * piece, width)
        r.columns[a:b] = dot_t(rows, weights).astype(jnp.bfloat16).reshape(b - a, count, 4 * piece)
        for distance in reversed(chunk):
            for y, x in ((1, 1), (0, 1), (1, 0), (0, 0)):
                if (distance, y, x) == (0, 0, 0):
                    r.joined[place.chip] = r.columns[place.slot()]
                    continue
                copy = remote(
                    r.columns.at[place.slot(distance, y, x)],
                    r.joined.at[place.chip],
                    r.out_sems.at[len(sent)],
                    r.in_sems.at[place.chip],
                    place.at(distance, y, x),
                )
                copy.start()
                sent.append(copy)
    expert_swaps = [
        remote(ref, into.at[core], r.swap_send.at[4 + i], r.swap_recv.at[4 + i], place.partner)
        for i, (ref, into) in enumerate(experts)
    ]
    for swap in expert_swaps:
        swap.start()
    for load in loads[2:]:
        load.wait()
    decay = jnp.exp(
        -r.scale[...] * jax.nn.softplus(dot_t(normed, r.w_decay[...]) + r.bias[...])
    )
    strength = jax.nn.sigmoid(dot_t(normed, r.w_beta[...]))
    for h in range(heads):
        r.keep[h] = jnp.broadcast_to(decay[:, h : h + 1], (count, HD))
        r.beta[h] = jnp.broadcast_to(strength[:, h : h + 1], (count, HD))
    r.rows_two[place.slot(), :, width:] = share_rows(r.routes[...], r.logits[...])
    late_loads[0].wait()
    late_loads[1].wait()
    group = heads // layers
    down = lax.broadcasted_iota(jnp.int32, (count, HD), 0)
    for distance in range(layers):
        layer = flipped(place.z, distance)
        for y, x in ((0, 0), (0, 1), (1, 0), (1, 1)):
            if (distance, y, x) != (0, 0, 0):
                source = place.at(distance, y, x) // 2
                remote(
                    r.columns.at[0],
                    r.joined.at[source],
                    r.out_sems.at[0],
                    r.in_sems.at[source],
                    place.partner,
                ).wait_recv()
        own_heads = pl.ds(group * layer, group)
        joined = r.joined.at[pl.ds(4 * layer, 4)]
        query = jax.nn.silu(all_heads(joined, group, 0, piece))
        query = query * inverse_norm(query) * HD ** (-0.5)
        keys = jax.nn.silu(all_heads(joined, group, 1, piece))
        keys = keys * inverse_norm(keys)
        r.keys[own_heads] = keys
        asks = jnp.concatenate([keys, query], axis=1).astype(jnp.bfloat16)
        overlap = jnp.sum(keys * query, axis=-1, keepdims=True)
        guesses, sights = [], []
        for h in range(group):
            guess = jnp.zeros((count, HD), jnp.float32)
            seen = jnp.zeros((count, HD), jnp.float32)
            for i in range(count):
                both = jnp.dot(
                    asks[h], r.state[i, group * layer + h], preferred_element_type=jnp.float32
                )
                guess = jnp.where(down == i, both[0:count], guess)
                seen = jnp.where(down == i, both[count:], seen)
            guesses.append(guess)
            sights.append(seen)
        keep = r.keep[own_heads]
        values = jax.nn.silu(all_heads(joined, group, 2, piece))
        change = r.beta[own_heads] * (values - keep * jnp.stack(guesses))
        r.change[own_heads] = change
        output = rms_scale(keep * jnp.stack(sights) + overlap * change) * r.head_gain[...]
        mixed = (output * jax.nn.silu(all_heads(joined, group, 3, piece))).astype(jnp.bfloat16)
        mixed = jnp.concatenate([mixed[h] for h in range(group)], axis=1)
        rows = pl.ds(pl.multiple_of(group * HD * layer, HD), group * HD)
        for j in range(0, width, 512):
            branch = jnp.dot(
                mixed, r.w_out[rows, j : j + 512], preferred_element_type=jnp.float32
            )
            if distance:
                branch = branch + r.x_second[:, j : j + 512]
            r.x_second[:, j : j + 512] = branch
    x_second = wide(r.x[...]) + rms_scale(r.x_second[...]) * r.gain_mix[...]
    r.x_second[...] = x_second
    r.rows_two[place.slot(), :, 0:width] = (rms_scale(x_second) * r.gain_pre[...]).astype(
        jnp.bfloat16
    )
    second = Gather(place, r.rows_two, r.two_send, r.two_recv)
    second.begin()

    def update(h, carry):
        upright = jnp.transpose(r.keys[h])
        change, keep = r.change[h], r.keep[h]
        for i in range(count):
            held = wide(r.state[i, h])
            key = jnp.broadcast_to(upright[:, i : i + 1], held.shape)
            r.new_state[i, h] = (keep[i : i + 1] * held + key * change[i : i + 1]).astype(
                jnp.bfloat16
            )
        return carry

    scatter = Scatter(
        place,
        r.parts,
        r.plane,
        r.column,
        (r.sum_send, r.plane_recv, r.column_recv),
    )
    plan = [heads * i // 16 for i in (0, 5, 11, 14, 16)]

    def fill(i):
        lax.fori_loop(plan[i], plan[i + 1], update, 0)

    fill(0)
    for step in second.relays():
        step()
    fill(1)

    def compute(chunk):
        a, b = 4 * chunk[0], 4 * (chunk[-1] + 1)
        number = (b - a) * count

        rows = r.rows_two[a:b, :, 0:width].reshape(number, width)
        share = wide(r.rows_two[a:b, :, width:]).reshape(number, LANES)
        lane = lax.rem(lax.broadcasted_iota(jnp.int32, share.shape, 1), HALF)
        share = jnp.sum(jnp.where(lane == place.me // PIECES, share, 0.0), axis=1, keepdims=True)
        for i in range(2):
            for j in range(0, hidden_units, 256):
                gated = clamped_unit(
                    jnp.dot(rows, r.gate[i, :, j : j + 256], preferred_element_type=jnp.float32),
                    jnp.dot(rows, r.up[i, :, j : j + 256], preferred_element_type=jnp.float32),
                )
                at = i * hidden_units + j
                r.hidden[0:number, at : at + 256] = gated.astype(jnp.bfloat16)
        units = r.hidden[0:number]
        for j in range(0, width, 512):
            weights = r.down[:, :, j : j + 512].reshape(2 * hidden_units, 512)
            part = jnp.dot(units, weights, preferred_element_type=jnp.float32)
            r.parts[a:b, :, j : j + 512] = (
                (part * share).astype(jnp.bfloat16).reshape(b - a, count, 512)
            )
        for distance in reversed(chunk):
            scatter.first(distance)

    for number, chunk in enumerate(chunks):
        for distance in chunk:
            second.across(distance)
        if not number:
            for load in late_loads[2:]:
                load.wait()
            for i, (ref, into) in enumerate(experts):
                remote(
                    ref, into.at[other], r.swap_send.at[4 + i], r.swap_recv.at[4 + i], place.partner
                ).wait_recv()
        compute(chunk)
    fill(2)
    for chunk in chunks:
        for distance in reversed(chunk):
            scatter.last(distance)
    fill(3)
    for distance in range(1, layers):
        scatter.collect(distance)
    r.result[...] = (r.x_second[...] + rms_scale(scatter.value) * r.gain_post[...]).astype(
        jnp.bfloat16
    )
    settle(
        gather.started + swaps + sent + expert_swaps + second.started + scatter.started
    )


def store_kernel(result, new_state, result_hbm, state_hbm, sems):
    pairs = [(new_state.at[i], state_hbm.at[i]) for i in range(new_state.shape[0])]
    for store in load_all([(result, result_hbm)] + pairs, sems):
        store.wait()


def shards(
    residual_in,
    gain_mix_pre,
    w_query,
    w_key,
    w_value,
    w_outgate,
    w_decay,
    w_beta,
    decay_scale,
    decay_bias,
    head_gain,
    w_out,
    gain_mix_post,
    state_cache,
    gain_ffn_pre,
    routes,
    route_logits,
    w_gate,
    w_up,
    w_down,
    gain_ffn_post,
):
    devices = lax.axis_size("ep")
    layers, pairs = devices // 8, devices // 2
    count, width = residual_in.shape
    heads = w_decay.shape[1]
    own = w_query.shape[1]
    units = w_gate.shape[1]
    rows = 4 * max(1, layers // 2) * count
    if layers > 1:
        rows = max(rows, 4 * (layers - layers // 2) * count)
    inputs = dict(
        x=residual_in,
        gain=gain_mix_pre[None],
        routes=routes.T,
        logits=route_logits.T,
        w_decay=w_decay.T,
        w_beta=w_beta.T,
        scale=decay_scale[None],
        bias=decay_bias[None],
        head_gain=head_gain[None],
        gain_mix=gain_mix_post[None],
        gain_pre=gain_ffn_pre[None],
        gain_post=gain_ffn_post[None],
        query=w_query.T,
        key=w_key.T,
        value=w_value.T,
        outgate=w_outgate.T,
        state=state_cache,
        w_out=w_out,
        gate=w_gate,
        up=w_up,
        down=w_down,
    )
    bf16, f32 = jnp.bfloat16, jnp.float32
    dma = pltpu.SemaphoreType.DMA

    def blocks(number, lanes=width):
        return pltpu.VMEM((number, count, lanes), bf16)

    def per_head():
        return pltpu.VMEM((heads, count, HD), f32)

    scratch = {name: pltpu.VMEM(inputs[name].shape, inputs[name].dtype) for name in SMALL}
    scratch |= dict(
        weights=pltpu.VMEM((4, 2, own, width), bf16),
        state=pltpu.VMEM(state_cache.shape, bf16),
        w_out=pltpu.VMEM(w_out.shape, bf16),
        gate=pltpu.VMEM((2,) + w_gate.shape, bf16),
        up=pltpu.VMEM((2,) + w_up.shape, bf16),
        down=pltpu.VMEM((2,) + w_down.shape, bf16),
        rows_one=blocks(pairs),
        rows_two=blocks(pairs, width + LANES),
        columns=blocks(pairs, 8 * own),
        joined=blocks(pairs, 8 * own),
        keys=per_head(),
        keep=per_head(),
        beta=per_head(),
        change=per_head(),
        x_second=pltpu.VMEM((count, width), f32),
        hidden=pltpu.VMEM((rows, 2 * units), bf16),
        parts=blocks(pairs),
        plane=blocks(3 * layers),
        column=blocks(layers),
        small_sems=dma((len(SMALL),)),
        weight_sems=dma((4,)),
        late_sems=dma((5,)),
        swap_send=dma((7,)),
        swap_recv=dma((7,)),
        one_send=dma((gather_sends(devices),)),
        one_recv=dma((pairs,)),
        two_send=dma((gather_sends(devices),)),
        two_recv=dma((pairs,)),
        out_sems=dma((pairs,)),
        in_sems=dma((pairs,)),
        sum_send=dma((4 * layers,)),
        plane_recv=dma((3 * layers,)),
        column_recv=dma((layers,)),
    )
    names = [name + "_hbm" for name in INPUTS] + ["result", "new_state"] + list(scratch)
    vmem = pl.BlockSpec(memory_space=pltpu.VMEM)
    hbm = pl.BlockSpec(memory_space=pltpu.HBM)
    held = pl.pallas_call(
        functools.partial(decode_kernel, devices, names),
        out_shape=(
            pltpu.VMEM((count, width), bf16),
            pltpu.VMEM(state_cache.shape, bf16),
        ),
        in_specs=[hbm] * len(INPUTS),
        out_specs=(vmem, vmem),
        scratch_shapes=list(scratch.values()),
        compiler_params=pltpu.CompilerParams(
            collective_id=0, has_side_effects=True, vmem_limit_bytes=VMEM_LIMIT
        ),
    )(*[inputs[name] for name in INPUTS])
    return pl.pallas_call(
        store_kernel,
        out_shape=[jax.ShapeDtypeStruct(a.shape, a.dtype) for a in held],
        in_specs=[vmem] * 2,
        out_specs=[hbm] * 2,
        scratch_shapes=[dma((count + 1,))],
        compiler_params=pltpu.CompilerParams(vmem_limit_bytes=1000 * 1000),
    )(*held)


def solution(mesh):
    in_specs = (
        P("ep", None),
        P(),
        P(None, "ep"),
        P(None, "ep"),
        P(None, "ep"),
        P(None, "ep"),
        P(),
        P(),
        P(),
        P(),
        P(),
        P(),
        P(),
        P("ep", None, None, None),
        P(),
        P("ep", None),
        P("ep", None),
        P(None, "ep"),
        P(None, "ep"),
        P("ep", None),
        P(),
    )
    out_specs = (P("ep", None), P("ep", None, None, None))
    return jax.shard_map(shards, mesh=mesh, in_specs=in_specs, out_specs=out_specs, check_vma=False)
```

```python
import functools
import types

import jax
import jax.numpy as jnp
from jax import lax
from jax.experimental import pallas as pl
from jax.experimental.pallas import tpu as pltpu
from jax.sharding import PartitionSpec as P

H = 16
HD = 128
PIECES = 4
TOPK = 4
LANES = 128
HALF = LANES // 2
SUM_CUTS = 2
VMEM_LIMIT = 58 * 1000 * 1000
MESH = pl.DeviceIdType.MESH

EPS = 1e-06
LIMIT = 7.0
ALPHA = 1.702


def rms_scale(values):
    return values * lax.rsqrt(jnp.mean(values * values, axis=-1, keepdims=True) + EPS)


def clamped_unit(gate, upper):
    glu = jnp.minimum(gate, LIMIT)
    linear = jnp.clip(upper, -LIMIT, LIMIT)
    return glu * jax.nn.sigmoid(ALPHA * glu) * (linear + 1.0)


def flipped(value, distance):
    bit = 1
    while bit <= distance:
        if distance & bit:
            value = value + bit - 2 * bit * (lax.rem(value // bit, 2))
        bit *= 2
    return value


class Place:
    def __init__(self, devices):
        self.layers = devices // 8
        self.me = lax.axis_index("ep")
        self.core = lax.rem(self.me, 2)
        self.x = lax.rem(self.me // 2, 2)
        self.y = lax.rem(self.me // 4, 2)
        self.z = self.me // 8
        self.chip = self.me // 2
        self.partner = flipped(self.me, 1)

    def at(self, distance=0, y=0, x=0):
        z = flipped(self.z, distance)
        return z * 8 + flipped(self.y, y) * 4 + flipped(self.x, x) * 2 + self.core

    def slot(self, distance=0, y=0, x=0):
        return distance * 4 + flipped(self.y, y) * 2 + flipped(self.x, x)


def greet(partners):
    barrier = pltpu.get_barrier_semaphore()
    for partner in partners:
        pl.semaphore_signal(barrier, inc=1, device_id=(partner,), device_id_type=MESH)
    return lambda: pl.semaphore_wait(barrier, len(partners))


def remote(source, target, send_sem, recv_sem, device):
    return pltpu.make_async_remote_copy(
        src_ref=source,
        dst_ref=target,
        send_sem=send_sem,
        recv_sem=recv_sem,
        device_id=(device,),
        device_id_type=MESH,
    )


PLANE = ((1, 1), (0, 1), (1, 0))


def lanes_of(ref, cuts):
    width = ref.shape[-1]
    bounds = [width // LANES * i // cuts * LANES for i in range(cuts + 1)]
    return [pl.ds(a, b - a) for a, b in zip(bounds, bounds[1:])]


def chunks_of(layers):
    half = max(1, layers // 2)
    return [c for c in (range(0, half), range(half, layers)) if len(c)]


class Gather:
    def __init__(self, place, buf, send_sem, column_recv, plane_recv):
        self.place, self.buf = place, buf
        self.send_sem, self.column_recv, self.plane_recv = send_sem, column_recv, plane_recv
        self.sends = 0
        self.chunks = chunks_of(place.layers)

    def push(self, source, target, recv_sem, device):
        remote(
            self.buf.at[source], self.buf.at[target], self.send_sem.at[0], recv_sem, device
        ).start()
        self.sends += 1

    def arrive(self, blocks, recv_sem):
        remote(blocks, blocks, self.send_sem.at[0], recv_sem, self.place.partner).wait_recv()

    def spread(self, distance):
        place = self.place
        slot = place.slot(distance)
        sem = self.plane_recv.at[[distance in chunk for chunk in self.chunks].index(True)]
        for y, x in PLANE:
            self.push(slot, slot, sem, place.at(y=y, x=x))

    def column(self, distance):
        slot = self.place.slot(distance)
        self.arrive(self.buf.at[slot], self.column_recv.at[distance])
        self.spread(distance)

    def across(self, number):
        blocks = 3 * len(self.chunks[number])
        self.arrive(self.buf.at[pl.ds(0, blocks)], self.plane_recv.at[number])

    def begin(self):
        place = self.place
        for distance in range(1, place.layers):
            self.push(
                place.slot(),
                place.slot(distance),
                self.column_recv.at[distance],
                place.at(distance),
            )
        self.spread(0)

    def relays(self):
        return [functools.partial(self.column, d) for d in range(1, self.place.layers)]

    def settle(self):
        settle(self.buf.at[pl.ds(0, self.sends)], self.send_sem.at[0], self.place.partner)


class Scatter:
    def __init__(self, place, parts, plane, column, cuts, sems):
        self.place, self.parts = place, parts
        self.plane, self.column = plane, column
        self.lanes = lanes_of(parts, cuts)
        self.send_sem, self.plane_recv, self.column_recv = sems
        self.sends = 0
        self.values = [None] * cuts

    def push(self, source, target, recv_sem, device):
        remote(source, target, self.send_sem.at[0], recv_sem, device).start()
        self.sends += 1

    def arrive(self, blocks, recv_sem):
        remote(blocks, blocks, self.send_sem.at[0], recv_sem, self.place.partner).wait_recv()

    def first(self, distance, cut):
        place, lanes = self.place, self.lanes[cut]
        for i, (y, x) in enumerate(PLANE):
            self.push(
                self.parts.at[place.slot(distance, y, x), :, lanes],
                self.plane.at[3 * distance + i, :, lanes],
                self.plane_recv.at[distance, cut],
                place.at(y=y, x=x),
            )

    def last(self, distance, cut):
        place, lanes = self.place, self.lanes[cut]
        slot = place.slot(distance)
        value = wide(self.parts[slot, :, lanes])
        self.arrive(
            self.plane.at[pl.ds(3 * distance, 3), :, lanes], self.plane_recv.at[distance, cut]
        )
        for i in reversed(range(3)):
            value = value + wide(self.plane[3 * distance + i, :, lanes])
        if distance > 0:
            self.parts[slot, :, lanes] = value.astype(jnp.bfloat16)
            self.push(
                self.parts.at[slot, :, lanes],
                self.column.at[distance - 1, :, lanes],
                self.column_recv.at[cut],
                place.at(distance),
            )
        else:
            self.values[cut] = value

    def collect(self, cut):
        lanes = self.lanes[cut]
        others = self.place.layers - 1
        if others:
            self.arrive(self.column.at[pl.ds(0, others), :, lanes], self.column_recv.at[cut])
        for i in range(others):
            self.values[cut] = self.values[cut] + wide(self.column[i, :, lanes])

    def settle(self):
        blocks = self.sends // len(self.lanes)
        settle(self.parts.at[pl.ds(0, blocks)], self.send_sem.at[0], self.place.partner)


def settle(blocks, send_sem, partner):
    remote(blocks, blocks, send_sem, send_sem, partner).wait_send()


def landed(blocks, sem):
    pltpu.make_async_copy(blocks, blocks, sem).wait()


def wide(block):
    return block.astype(jnp.float32)


def dot_t(left, right):
    return lax.dot_general(
        left, right, (((1,), (1,)), ((), ())), preferred_element_type=jnp.float32
    )


def column_of(row):
    size = row.shape[1]
    across = lax.broadcasted_iota(jnp.int32, (size, size), 1)
    down = lax.broadcasted_iota(jnp.int32, (size, size), 0)
    return jnp.sum(
        jnp.where(across == down, jnp.broadcast_to(row, (size, size)), 0.0), axis=1, keepdims=True
    )


def share_rows(routes, logits):
    raised = jnp.exp(logits)
    shares = raised / jnp.sum(raised, axis=0, keepdims=True)
    routes = routes.astype(jnp.float32)
    count = routes.shape[1]
    lane = lax.broadcasted_iota(jnp.int32, (count, LANES), 1)
    expert = lax.rem(lane, HALF).astype(jnp.float32)
    share = jnp.zeros((count, LANES), jnp.float32)
    for j in range(routes.shape[0]):
        share = share + jnp.where(
            expert == column_of(routes[j : j + 1]), column_of(shares[j : j + 1]), 0.0
        )
    high = share.astype(jnp.bfloat16)
    low = (share - wide(high)).astype(jnp.bfloat16)
    return jnp.where(lane < HALF, wide(high), wide(low)).astype(jnp.bfloat16)


def head_rows(joined, head, kind, piece):
    lane = lax.broadcasted_iota(jnp.int32, (joined.shape[1], LANES), 1)
    value = jnp.zeros(lane.shape, jnp.float32)
    group, offset = divmod(kind * piece, LANES)
    for i in range(HD // piece):
        part = joined[head * (HD // piece) + i, :, group * LANES : (group + 1) * LANES]
        part = wide(part)
        shift = (i * piece - offset) % LANES
        if shift:
            part = pltpu.roll(part, shift, 1)
        value = jnp.where((lane >= i * piece) & (lane < (i + 1) * piece), part, value)
    return value


def all_heads(joined, heads, kind, piece):
    if piece == HD:
        return wide(joined[:, :, kind * HD : (kind + 1) * HD])
    return jnp.stack([head_rows(joined, head, kind, piece) for head in range(heads)])


def inverse_norm(values):
    return lax.rsqrt(jnp.sum(values * values, axis=-1, keepdims=True) + EPS)


GROUPS = dict(
    x=("x",),
    gain=("gain",),
    routes=("routes",),
    logits=("logits",),
    rates=("w_decay", "w_beta"),
    decays=("scale", "bias"),
    head_gain=("head_gain",),
    gains=("gain_mix", "gain_pre", "gain_post"),
    weights=("query", "key", "value", "outgate"),
    state=("state",),
    w_out=("w_out",),
    wide_in=("gate", "up"),
    down=("down",),
)
INPUTS = tuple(name for group in GROUPS.values() for name in group)
PAIRED = ("weights", "wide_in", "down")
LATE = ("state", "w_out", "wide_in", "down")


def decode_kernel(devices, names, *refs):
    r = types.SimpleNamespace(**dict(zip(names, refs)))
    place = Place(devices)
    layers, pairs = place.layers, devices // 2
    core, other = place.core, 1 - place.core
    count, width = r.x.shape
    heads = r.keys.shape[0]
    piece = 2 * r.query_hbm.shape[0]
    hidden_units = r.gate_hbm.shape[1]
    chunks = chunks_of(layers)

    def target(group, i):
        into = getattr(r, group)
        if group in PAIRED:
            return into.at[i, core]
        return into if len(GROUPS[group]) == 1 else into.at[i]

    def load(groups):
        for group in groups:
            for i, name in enumerate(GROUPS[group]):
                pltpu.make_async_copy(
                    getattr(r, name + "_hbm"), target(group, i), r.load_sems.at[order[group]]
                ).start()

    def loaded(group):
        into = getattr(r, group)
        landed(into.at[:, core] if group in PAIRED else into, r.load_sems.at[order[group]])

    def swap(group):
        for i, name in enumerate(GROUPS[group]):
            at = PAIRED.index(group)
            remote(
                getattr(r, name + "_hbm"),
                target(group, i),
                r.swap_send.at[at],
                r.swap_recv.at[at],
                place.partner,
            ).start()

    def swapped(group):
        at = PAIRED.index(group)
        into = getattr(r, group).at[:, other]
        remote(into, into, r.swap_send.at[at], r.swap_recv.at[at], place.partner).wait_recv()

    def swaps_settle(groups):
        for group in groups:
            into = getattr(r, group).at[:, core]
            settle(into, r.swap_send.at[PAIRED.index(group)], place.partner)

    order = {group: i for i, group in enumerate(GROUPS)}
    ready = greet(
        [place.at(distance) for distance in range(1, layers)]
        + [place.at(y=y, x=x) for y, x in PLANE]
        + [place.partner]
    )
    load(group for group in GROUPS if group not in LATE)
    loaded("x")
    loaded("gain")
    normed = (rms_scale(wide(r.x[...])) * r.gain[...]).astype(jnp.bfloat16)
    gather = Gather(place, r.rows_one, r.one_send, r.one_column, r.one_plane)
    r.rows_one[place.slot()] = normed
    ready()
    gather.begin()
    swap("weights")
    load(LATE)
    for step in gather.relays():
        step()
    for number, chunk in enumerate(chunks):
        gather.across(number)
        if not number:
            loaded("weights")
            swapped("weights")
        a, b = 4 * chunk[0], 4 * (chunk[-1] + 1)
        rows = r.rows_one[a:b].reshape((b - a) * count, width)
        weights = r.weights[...].reshape(4 * piece, width)
        r.columns[a:b] = dot_t(rows, weights).astype(jnp.bfloat16).reshape(b - a, count, 4 * piece)
        for distance in reversed(chunk):
            for y, x in ((1, 1), (0, 1), (1, 0), (0, 0)):
                if (distance, y, x) == (0, 0, 0):
                    r.joined[place.chip] = r.columns[place.slot()]
                    continue
                remote(
                    r.columns.at[place.slot(distance, y, x)],
                    r.joined.at[place.chip],
                    r.out_sem.at[0],
                    r.in_sems.at[distance],
                    place.at(distance, y, x),
                ).start()
    swap("wide_in")
    swap("down")
    for group in ("routes", "logits", "rates", "decays", "head_gain", "gains"):
        loaded(group)
    decay = jnp.exp(
        -r.decays[0] * jax.nn.softplus(dot_t(normed, r.rates[0]) + r.decays[1])
    )
    strength = jax.nn.sigmoid(dot_t(normed, r.rates[1]))
    for h in range(heads):
        r.keep[h] = jnp.broadcast_to(decay[:, h : h + 1], (count, HD))
        r.beta[h] = jnp.broadcast_to(strength[:, h : h + 1], (count, HD))
    r.rows_two[place.slot(), :, width:] = share_rows(r.routes[...], r.logits[...])
    loaded("state")
    loaded("w_out")
    group = heads // layers
    down = lax.broadcasted_iota(jnp.int32, (count, HD), 0)
    for distance in range(layers):
        layer = flipped(place.z, distance)
        blocks = r.joined.at[pl.ds(0, 4 if distance else 3)]
        remote(
            blocks, blocks, r.out_sem.at[0], r.in_sems.at[distance], place.partner
        ).wait_recv()
        own_heads = pl.ds(group * layer, group)
        joined = r.joined.at[pl.ds(4 * layer, 4)]
        query = jax.nn.silu(all_heads(joined, group, 0, piece))
        query = query * inverse_norm(query) * HD ** (-0.5)
        keys = jax.nn.silu(all_heads(joined, group, 1, piece))
        keys = keys * inverse_norm(keys)
        r.keys[own_heads] = keys
        asks = jnp.concatenate([keys, query], axis=1).astype(jnp.bfloat16)
        overlap = jnp.sum(keys * query, axis=-1, keepdims=True)
        guesses, sights = [], []
        for h in range(group):
            guess = jnp.zeros((count, HD), jnp.float32)
            seen = jnp.zeros((count, HD), jnp.float32)
            for i in range(count):
                both = jnp.dot(
                    asks[h], r.state[i, group * layer + h], preferred_element_type=jnp.float32
                )
                guess = jnp.where(down == i, both[0:count], guess)
                seen = jnp.where(down == i, both[count:], seen)
            guesses.append(guess)
            sights.append(seen)
        keep = r.keep[own_heads]
        values = jax.nn.silu(all_heads(joined, group, 2, piece))
        change = r.beta[own_heads] * (values - keep * jnp.stack(guesses))
        r.change[own_heads] = change
        output = rms_scale(keep * jnp.stack(sights) + overlap * change) * r.head_gain[...]
        mixed = (output * jax.nn.silu(all_heads(joined, group, 3, piece))).astype(jnp.bfloat16)
        mixed = jnp.concatenate([mixed[h] for h in range(group)], axis=1)
        rows = pl.ds(pl.multiple_of(group * HD * layer, HD), group * HD)
        for j in range(0, width, 512):
            branch = jnp.dot(
                mixed, r.w_out[rows, j : j + 512], preferred_element_type=jnp.float32
            )
            if distance:
                branch = branch + r.x_second[:, j : j + 512]
            r.x_second[:, j : j + 512] = branch
    x_second = wide(r.x[...]) + rms_scale(r.x_second[...]) * r.gains[0]
    r.x_second[...] = x_second
    r.rows_two[place.slot(), :, 0:width] = (rms_scale(x_second) * r.gains[1]).astype(
        jnp.bfloat16
    )
    second = Gather(place, r.rows_two, r.two_send, r.two_column, r.two_plane)
    second.begin()

    def update(h, carry):
        upright = jnp.transpose(r.keys[h])
        change, keep = r.change[h], r.keep[h]
        for i in range(count):
            held = wide(r.state[i, h])
            key = jnp.broadcast_to(upright[:, i : i + 1], held.shape)
            r.new_state[i, h] = (keep[i : i + 1] * held + key * change[i : i + 1]).astype(
                jnp.bfloat16
            )
        return carry

    scatter = Scatter(
        place,
        r.parts,
        r.plane,
        r.column,
        SUM_CUTS,
        (r.sum_send, r.plane_recv, r.column_recv),
    )
    plan = [heads * i // 16 for i in (0, 5, 9, 13, 16)]

    def fill(i):
        lax.fori_loop(plan[i], plan[i + 1], update, 0)

    fill(0)
    gather.settle()
    settle(r.columns.at[pl.ds(0, pairs - 1)], r.out_sem.at[0], place.partner)
    swaps_settle(("weights",))
    for step in second.relays():
        step()
    fill(1)

    def compute(chunk):
        a, b = 4 * chunk[0], 4 * (chunk[-1] + 1)
        number = (b - a) * count

        r.packed[0:number] = r.rows_two[a:b, :, 0:width].reshape(number, width)
        share = wide(r.rows_two[a:b, :, width:]).reshape(number, LANES)
        lane = lax.rem(lax.broadcasted_iota(jnp.int32, share.shape, 1), HALF)
        share = jnp.sum(jnp.where(lane == place.me // PIECES, share, 0.0), axis=1, keepdims=True)
        for i in range(2):
            for j in range(0, hidden_units, LANES):
                rows = r.packed[0:number]
                gated = clamped_unit(
                    jnp.dot(rows, r.wide_in[0, i, :, j : j + LANES], preferred_element_type=jnp.float32),
                    jnp.dot(rows, r.wide_in[1, i, :, j : j + LANES], preferred_element_type=jnp.float32),
                )
                at = i * hidden_units + j
                r.hidden[0:number, at : at + LANES] = gated.astype(jnp.bfloat16)
        for cut, lanes in enumerate(scatter.lanes):
            for j in range(lanes.start, lanes.start + lanes.size, LANES):
                weights = r.down[0, :, :, j : j + LANES].reshape(2 * hidden_units, LANES)
                units = r.hidden[0:number]
                part = jnp.dot(units, weights, preferred_element_type=jnp.float32)
                r.parts[a:b, :, j : j + LANES] = (
                    (part * share).astype(jnp.bfloat16).reshape(b - a, count, LANES)
                )
            for distance in reversed(chunk):
                scatter.first(distance, cut)

    for number, chunk in enumerate(chunks):
        second.across(number)
        if not number:
            for group in ("wide_in", "down"):
                loaded(group)
                swapped(group)
        compute(chunk)
    fill(2)
    second.settle()
    swaps_settle(("wide_in", "down"))
    for chunk in chunks:
        for cut in range(SUM_CUTS):
            for distance in reversed(chunk):
                scatter.last(distance, cut)
    fill(3)
    for cut in range(SUM_CUTS):
        scatter.collect(cut)
    moe = jnp.concatenate(scatter.values, axis=1)
    r.result[...] = (r.x_second[...] + rms_scale(moe) * r.gains[2]).astype(
        jnp.bfloat16
    )
    scatter.settle()


def store_kernel(result, new_state, result_hbm, state_hbm, sems):
    store = pltpu.make_async_copy(result, result_hbm, sems.at[0])
    store.start()
    for i in range(new_state.shape[0]):
        pltpu.make_async_copy(new_state.at[i], state_hbm.at[i], sems.at[1]).start()
    store.wait()
    pltpu.make_async_copy(new_state, state_hbm, sems.at[1]).wait()


def shards(
    residual_in,
    gain_mix_pre,
    w_query,
    w_key,
    w_value,
    w_outgate,
    w_decay,
    w_beta,
    decay_scale,
    decay_bias,
    head_gain,
    w_out,
    gain_mix_post,
    state_cache,
    gain_ffn_pre,
    routes,
    route_logits,
    w_gate,
    w_up,
    w_down,
    gain_ffn_post,
):
    devices = lax.axis_size("ep")
    layers, pairs = devices // 8, devices // 2
    count, width = residual_in.shape
    heads = w_decay.shape[1]
    own = w_query.shape[1]
    units = w_gate.shape[1]
    rows = 4 * max(1, layers // 2) * count
    if layers > 1:
        rows = max(rows, 4 * (layers - layers // 2) * count)
    inputs = dict(
        x=residual_in,
        gain=gain_mix_pre[None],
        routes=routes.T,
        logits=route_logits.T,
        w_decay=w_decay.T,
        w_beta=w_beta.T,
        scale=decay_scale[None],
        bias=decay_bias[None],
        head_gain=head_gain[None],
        gain_mix=gain_mix_post[None],
        gain_pre=gain_ffn_pre[None],
        gain_post=gain_ffn_post[None],
        query=w_query.T,
        key=w_key.T,
        value=w_value.T,
        outgate=w_outgate.T,
        state=state_cache,
        w_out=w_out,
        gate=w_gate,
        up=w_up,
        down=w_down,
    )
    bf16, f32 = jnp.bfloat16, jnp.float32
    dma = pltpu.SemaphoreType.DMA

    def blocks(number, lanes=width):
        return pltpu.VMEM((number, count, lanes), bf16)

    def per_head():
        return pltpu.VMEM((heads, count, HD), f32)

    def stacked(group):
        first = inputs[GROUPS[group][0]]
        pair = (2,) if group in PAIRED else ()
        many = (len(GROUPS[group]),) if group in PAIRED or len(GROUPS[group]) > 1 else ()
        return pltpu.VMEM(many + pair + first.shape, first.dtype)

    scratch = {group: stacked(group) for group in GROUPS}
    scratch |= dict(
        rows_one=blocks(pairs),
        rows_two=blocks(pairs, width + LANES),
        columns=blocks(pairs, 8 * own),
        joined=blocks(pairs, 8 * own),
        keys=per_head(),
        keep=per_head(),
        beta=per_head(),
        change=per_head(),
        x_second=pltpu.VMEM((count, width), f32),
        hidden=pltpu.VMEM((rows, 2 * units), bf16),
        packed=pltpu.VMEM((rows, width), bf16),
        parts=blocks(pairs),
        plane=blocks(3 * layers),
        column=blocks(layers),
        load_sems=dma((len(GROUPS),)),
        swap_send=dma((len(PAIRED),)),
        swap_recv=dma((len(PAIRED),)),
        one_send=dma((1,)),
        one_column=dma((layers,)),
        one_plane=dma((len(chunks_of(layers)),)),
        two_send=dma((1,)),
        two_column=dma((layers,)),
        two_plane=dma((len(chunks_of(layers)),)),
        out_sem=dma((1,)),
        in_sems=dma((layers,)),
        sum_send=dma((1,)),
        plane_recv=dma((layers, SUM_CUTS)),
        column_recv=dma((SUM_CUTS,)),
    )
    names = [name + "_hbm" for name in INPUTS] + ["result", "new_state"] + list(scratch)
    vmem = pl.BlockSpec(memory_space=pltpu.VMEM)
    hbm = pl.BlockSpec(memory_space=pltpu.HBM)
    held = pl.pallas_call(
        functools.partial(decode_kernel, devices, names),
        out_shape=(
            pltpu.VMEM((count, width), bf16),
            pltpu.VMEM(state_cache.shape, bf16),
        ),
        in_specs=[hbm] * len(INPUTS),
        out_specs=(vmem, vmem),
        scratch_shapes=list(scratch.values()),
        compiler_params=pltpu.CompilerParams(
            collective_id=0, has_side_effects=True, vmem_limit_bytes=VMEM_LIMIT
        ),
    )(*[inputs[name] for name in INPUTS])
    return pl.pallas_call(
        store_kernel,
        out_shape=[jax.ShapeDtypeStruct(a.shape, a.dtype) for a in held],
        in_specs=[vmem] * 2,
        out_specs=[hbm] * 2,
        scratch_shapes=[dma((2,))],
        compiler_params=pltpu.CompilerParams(vmem_limit_bytes=1000 * 1000),
    )(*held)


def solution(mesh):
    in_specs = (
        P("ep", None),
        P(),
        P(None, "ep"),
        P(None, "ep"),
        P(None, "ep"),
        P(None, "ep"),
        P(),
        P(),
        P(),
        P(),
        P(),
        P(),
        P(),
        P("ep", None, None, None),
        P(),
        P("ep", None),
        P("ep", None),
        P(None, "ep"),
        P(None, "ep"),
        P("ep", None),
        P(),
    )
    out_specs = (P("ep", None), P("ep", None, None, None))
    return jax.shard_map(shards, mesh=mesh, in_specs=in_specs, out_specs=out_specs, check_vma=False)
```

```python
import functools
import types

import jax
import jax.numpy as jnp
from jax import lax
from jax.experimental import pallas as pl
from jax.experimental.pallas import tpu as pltpu
from jax.sharding import PartitionSpec as P

H = 16
HD = 128
PIECES = 4
TOPK = 4
LANES = 128
HALF = LANES // 2
SUM_CUTS = 2
VMEM_LIMIT = 58 * 1000 * 1000
MESH = pl.DeviceIdType.MESH

EPS = 1e-06
LIMIT = 7.0
ALPHA = 1.702


def rms_scale(values):
    return values * lax.rsqrt(jnp.mean(values * values, axis=-1, keepdims=True) + EPS)


def clamped_unit(gate, upper):
    glu = jnp.minimum(gate, LIMIT)
    linear = jnp.clip(upper, -LIMIT, LIMIT)
    return glu * jax.nn.sigmoid(ALPHA * glu) * (linear + 1.0)


def flipped(value, distance):
    bit = 1
    while bit <= distance:
        if distance & bit:
            value = value + bit - 2 * bit * (lax.rem(value // bit, 2))
        bit *= 2
    return value


class Place:
    def __init__(self, devices):
        self.layers = devices // 8
        self.me = lax.axis_index("ep")
        self.core = lax.rem(self.me, 2)
        self.x = lax.rem(self.me // 2, 2)
        self.y = lax.rem(self.me // 4, 2)
        self.z = self.me // 8
        self.chip = self.me // 2
        self.partner = flipped(self.me, 1)

    def at(self, distance=0, y=0, x=0):
        z = flipped(self.z, distance)
        return z * 8 + flipped(self.y, y) * 4 + flipped(self.x, x) * 2 + self.core

    def slot(self, distance=0, y=0, x=0):
        return distance * 4 + flipped(self.y, y) * 2 + flipped(self.x, x)


def greet(partners):
    barrier = pltpu.get_barrier_semaphore()
    for partner in partners:
        pl.semaphore_signal(barrier, inc=1, device_id=(partner,), device_id_type=MESH)
    return lambda: pl.semaphore_wait(barrier, len(partners))


def remote(source, target, send_sem, recv_sem, device):
    return pltpu.make_async_remote_copy(
        src_ref=source,
        dst_ref=target,
        send_sem=send_sem,
        recv_sem=recv_sem,
        device_id=(device,),
        device_id_type=MESH,
    )


PLANE = ((1, 1), (0, 1), (1, 0))


def lanes_of(ref, cuts):
    width = ref.shape[-1]
    bounds = [width // LANES * i // cuts * LANES for i in range(cuts + 1)]
    return [pl.ds(a, b - a) for a, b in zip(bounds, bounds[1:])]


def chunks_of(layers):
    half = max(1, layers // 2)
    return [c for c in (range(0, half), range(half, layers)) if len(c)]


class Gather:
    def __init__(self, place, buf, send_sem, column_recv, plane_recv):
        self.place, self.buf = place, buf
        self.send_sem, self.column_recv, self.plane_recv = send_sem, column_recv, plane_recv
        self.sends = 0
        self.chunks = chunks_of(place.layers)

    def push(self, source, target, recv_sem, device):
        remote(
            self.buf.at[source], self.buf.at[target], self.send_sem.at[0], recv_sem, device
        ).start()
        self.sends += 1

    def arrive(self, blocks, recv_sem):
        remote(blocks, blocks, self.send_sem.at[0], recv_sem, self.place.partner).wait_recv()

    def spread(self, distance):
        place = self.place
        slot = place.slot(distance)
        sem = self.plane_recv.at[[distance in chunk for chunk in self.chunks].index(True)]
        for y, x in PLANE:
            self.push(slot, slot, sem, place.at(y=y, x=x))

    def column(self, distance):
        slot = self.place.slot(distance)
        self.arrive(self.buf.at[slot], self.column_recv.at[distance])
        self.spread(distance)

    def across(self, number):
        blocks = 3 * len(self.chunks[number])
        self.arrive(self.buf.at[pl.ds(0, blocks)], self.plane_recv.at[number])

    def begin(self):
        place = self.place
        for distance in range(1, place.layers):
            self.push(
                place.slot(),
                place.slot(distance),
                self.column_recv.at[distance],
                place.at(distance),
            )
        self.spread(0)

    def relays(self):
        return [functools.partial(self.column, d) for d in range(1, self.place.layers)]

    def settle(self):
        settle(self.buf.at[pl.ds(0, self.sends)], self.send_sem.at[0], self.place.partner)


class Scatter:
    def __init__(self, place, parts, plane, column, cuts, sems):
        self.place, self.parts = place, parts
        self.plane, self.column = plane, column
        self.lanes = lanes_of(parts, cuts)
        self.send_sem, self.plane_recv, self.column_recv = sems
        self.sends = 0
        self.values = [None] * cuts

    def push(self, source, target, recv_sem, device):
        remote(source, target, self.send_sem.at[0], recv_sem, device).start()
        self.sends += 1

    def arrive(self, blocks, recv_sem):
        remote(blocks, blocks, self.send_sem.at[0], recv_sem, self.place.partner).wait_recv()

    def first(self, distance, cut):
        place, lanes = self.place, self.lanes[cut]
        for i, (y, x) in enumerate(PLANE):
            self.push(
                self.parts.at[place.slot(distance, y, x), :, lanes],
                self.plane.at[3 * distance + i, :, lanes],
                self.plane_recv.at[distance, cut],
                place.at(y=y, x=x),
            )

    def last(self, distance, cut):
        place, lanes = self.place, self.lanes[cut]
        slot = place.slot(distance)
        value = wide(self.parts[slot, :, lanes])
        self.arrive(
            self.plane.at[pl.ds(3 * distance, 3), :, lanes], self.plane_recv.at[distance, cut]
        )
        for i in reversed(range(3)):
            value = value + wide(self.plane[3 * distance + i, :, lanes])
        if distance > 0:
            self.parts[slot, :, lanes] = value.astype(jnp.bfloat16)
            self.push(
                self.parts.at[slot, :, lanes],
                self.column.at[distance - 1, :, lanes],
                self.column_recv.at[cut],
                place.at(distance),
            )
        else:
            self.values[cut] = value

    def collect(self, cut):
        lanes = self.lanes[cut]
        others = self.place.layers - 1
        if others:
            self.arrive(self.column.at[pl.ds(0, others), :, lanes], self.column_recv.at[cut])
        for i in range(others):
            self.values[cut] = self.values[cut] + wide(self.column[i, :, lanes])

    def settle(self):
        blocks = self.sends // len(self.lanes)
        settle(self.parts.at[pl.ds(0, blocks)], self.send_sem.at[0], self.place.partner)


def settle(blocks, send_sem, partner):
    remote(blocks, blocks, send_sem, send_sem, partner).wait_send()


def landed(blocks, sem):
    pltpu.make_async_copy(blocks, blocks, sem).wait()


def wide(block):
    return block.astype(jnp.float32)


def dot_t(left, right):
    return lax.dot_general(
        left, right, (((1,), (1,)), ((), ())), preferred_element_type=jnp.float32
    )


def column_of(row):
    size = row.shape[1]
    across = lax.broadcasted_iota(jnp.int32, (size, size), 1)
    down = lax.broadcasted_iota(jnp.int32, (size, size), 0)
    return jnp.sum(
        jnp.where(across == down, jnp.broadcast_to(row, (size, size)), 0.0), axis=1, keepdims=True
    )


def share_rows(routes, logits):
    raised = jnp.exp(logits)
    shares = raised / jnp.sum(raised, axis=0, keepdims=True)
    routes = routes.astype(jnp.float32)
    count = routes.shape[1]
    lane = lax.broadcasted_iota(jnp.int32, (count, LANES), 1)
    expert = lax.rem(lane, HALF).astype(jnp.float32)
    share = jnp.zeros((count, LANES), jnp.float32)
    for j in range(routes.shape[0]):
        share = share + jnp.where(
            expert == column_of(routes[j : j + 1]), column_of(shares[j : j + 1]), 0.0
        )
    high = share.astype(jnp.bfloat16)
    low = (share - wide(high)).astype(jnp.bfloat16)
    return jnp.where(lane < HALF, wide(high), wide(low)).astype(jnp.bfloat16)


def head_rows(joined, head, kind, piece):
    lane = lax.broadcasted_iota(jnp.int32, (joined.shape[1], LANES), 1)
    value = jnp.zeros(lane.shape, jnp.float32)
    group, offset = divmod(kind * piece, LANES)
    for i in range(HD // piece):
        part = joined[head * (HD // piece) + i, :, group * LANES : (group + 1) * LANES]
        part = wide(part)
        shift = (i * piece - offset) % LANES
        if shift:
            part = pltpu.roll(part, shift, 1)
        value = jnp.where((lane >= i * piece) & (lane < (i + 1) * piece), part, value)
    return value


def all_heads(joined, heads, kind, piece):
    if piece == HD:
        return wide(joined[:, :, kind * HD : (kind + 1) * HD])
    return jnp.stack([head_rows(joined, head, kind, piece) for head in range(heads)])


def inverse_norm(values):
    return lax.rsqrt(jnp.sum(values * values, axis=-1, keepdims=True) + EPS)


GROUPS = dict(
    x=("x",),
    gain=("gain",),
    routes=("routes",),
    logits=("logits",),
    rates=("w_decay", "w_beta"),
    decays=("scale", "bias"),
    head_gain=("head_gain",),
    gains=("gain_mix", "gain_pre", "gain_post"),
    weights=("query", "key", "value", "outgate"),
    state=("state",),
    w_out=("w_out",),
    wide_in=("gate", "up"),
    down=("down",),
)
INPUTS = tuple(name for group in GROUPS.values() for name in group)
PAIRED = ("weights", "wide_in", "down")
LATE = ("state", "w_out", "wide_in", "down")


def decode_kernel(devices, names, *refs):
    r = types.SimpleNamespace(**dict(zip(names, refs)))
    place = Place(devices)
    layers, pairs = place.layers, devices // 2
    core, other = place.core, 1 - place.core
    count, width = r.x.shape
    heads = r.keys.shape[0]
    piece = 2 * r.query_hbm.shape[0]
    hidden_units = r.gate_hbm.shape[1]
    chunks = chunks_of(layers)

    def target(group, i):
        into = getattr(r, group)
        if group in PAIRED:
            return into.at[i, core]
        return into if len(GROUPS[group]) == 1 else into.at[i]

    def load(groups):
        for group in groups:
            for i, name in enumerate(GROUPS[group]):
                pltpu.make_async_copy(
                    getattr(r, name + "_hbm"), target(group, i), r.load_sems.at[order[group]]
                ).start()

    def loaded(group):
        into = getattr(r, group)
        landed(into.at[:, core] if group in PAIRED else into, r.load_sems.at[order[group]])

    def swap(group):
        for i, name in enumerate(GROUPS[group]):
            at = PAIRED.index(group)
            remote(
                getattr(r, name + "_hbm"),
                target(group, i),
                r.swap_send.at[at],
                r.swap_recv.at[at],
                place.partner,
            ).start()

    def swapped(group):
        at = PAIRED.index(group)
        into = getattr(r, group).at[:, other]
        remote(into, into, r.swap_send.at[at], r.swap_recv.at[at], place.partner).wait_recv()

    def swaps_settle(groups):
        for group in groups:
            into = getattr(r, group).at[:, core]
            settle(into, r.swap_send.at[PAIRED.index(group)], place.partner)

    order = {group: i for i, group in enumerate(GROUPS)}
    ready = greet(
        [place.at(distance) for distance in range(1, layers)]
        + [place.at(y=y, x=x) for y, x in PLANE]
        + [place.partner]
    )
    load(group for group in GROUPS if group not in LATE)
    loaded("x")
    loaded("gain")
    normed = (rms_scale(wide(r.x[...])) * r.gain[...]).astype(jnp.bfloat16)
    gather = Gather(place, r.rows_one, r.one_send, r.one_column, r.one_plane)
    r.rows_one[place.slot()] = normed
    ready()
    gather.begin()
    swap("weights")
    load(LATE)
    for step in gather.relays():
        step()
    loaded("weights")
    swapped("weights")
    for j in range(0, width, 256):
        r.upright[j : j + 256] = jnp.transpose(
            r.weights[:, :, :, j : j + 256].reshape(4 * piece, 256)
        )
    for number, chunk in enumerate(chunks):
        gather.across(number)
        a, b = 4 * chunk[0], 4 * (chunk[-1] + 1)
        rows = r.rows_one[a:b].reshape((b - a) * count, width)
        product = jnp.dot(rows, r.upright[...], preferred_element_type=jnp.float32)
        r.columns[a:b] = product.astype(jnp.bfloat16).reshape(b - a, count, 4 * piece)
        for distance in reversed(chunk):
            for y, x in ((1, 1), (0, 1), (1, 0), (0, 0)):
                if (distance, y, x) == (0, 0, 0):
                    r.joined[place.chip] = r.columns[place.slot()]
                    continue
                remote(
                    r.columns.at[place.slot(distance, y, x)],
                    r.joined.at[place.chip],
                    r.out_sem.at[0],
                    r.in_sems.at[distance],
                    place.at(distance, y, x),
                ).start()
    swap("wide_in")
    swap("down")
    for group in ("routes", "logits", "rates", "decays", "head_gain", "gains"):
        loaded(group)
    decay = jnp.exp(
        -r.decays[0] * jax.nn.softplus(dot_t(normed, r.rates[0]) + r.decays[1])
    )
    strength = jax.nn.sigmoid(dot_t(normed, r.rates[1]))
    for h in range(heads):
        r.keep[h] = jnp.broadcast_to(decay[:, h : h + 1], (count, HD))
        r.beta[h] = jnp.broadcast_to(strength[:, h : h + 1], (count, HD))
    r.rows_two[place.slot(), :, width:] = share_rows(r.routes[...], r.logits[...])
    loaded("state")
    loaded("w_out")
    group = heads // layers
    down = lax.broadcasted_iota(jnp.int32, (count, HD), 0)
    for distance in range(layers):
        layer = flipped(place.z, distance)
        blocks = r.joined.at[pl.ds(0, 4 if distance else 3)]
        remote(
            blocks, blocks, r.out_sem.at[0], r.in_sems.at[distance], place.partner
        ).wait_recv()
        own_heads = pl.ds(group * layer, group)
        joined = r.joined.at[pl.ds(4 * layer, 4)]
        query = jax.nn.silu(all_heads(joined, group, 0, piece))
        query = query * inverse_norm(query) * HD ** (-0.5)
        keys = jax.nn.silu(all_heads(joined, group, 1, piece))
        keys = keys * inverse_norm(keys)
        r.keys[own_heads] = keys
        asks = jnp.concatenate([keys, query], axis=1).astype(jnp.bfloat16)
        overlap = jnp.sum(keys * query, axis=-1, keepdims=True)
        guesses, sights = [], []
        for h in range(group):
            guess = jnp.zeros((count, HD), jnp.float32)
            seen = jnp.zeros((count, HD), jnp.float32)
            for i in range(count):
                both = jnp.dot(
                    asks[h], r.state[i, group * layer + h], preferred_element_type=jnp.float32
                )
                guess = jnp.where(down == i, both[0:count], guess)
                seen = jnp.where(down == i, both[count:], seen)
            guesses.append(guess)
            sights.append(seen)
        keep = r.keep[own_heads]
        values = jax.nn.silu(all_heads(joined, group, 2, piece))
        change = r.beta[own_heads] * (values - keep * jnp.stack(guesses))
        r.change[own_heads] = change
        output = rms_scale(keep * jnp.stack(sights) + overlap * change) * r.head_gain[...]
        mixed = (output * jax.nn.silu(all_heads(joined, group, 3, piece))).astype(jnp.bfloat16)
        mixed = jnp.concatenate([mixed[h] for h in range(group)], axis=1)
        rows = pl.ds(pl.multiple_of(group * HD * layer, HD), group * HD)
        for j in range(0, width, 512):
            branch = jnp.dot(
                mixed, r.w_out[rows, j : j + 512], preferred_element_type=jnp.float32
            )
            if distance:
                branch = branch + r.x_second[:, j : j + 512]
            r.x_second[:, j : j + 512] = branch
    x_second = wide(r.x[...]) + rms_scale(r.x_second[...]) * r.gains[0]
    r.x_second[...] = x_second
    r.rows_two[place.slot(), :, 0:width] = (rms_scale(x_second) * r.gains[1]).astype(
        jnp.bfloat16
    )
    second = Gather(place, r.rows_two, r.two_send, r.two_column, r.two_plane)
    def update(h, carry):
        upright = jnp.transpose(r.keys[h])
        change, keep = r.change[h], r.keep[h]
        for i in range(count):
            held = wide(r.state[i, h])
            key = jnp.broadcast_to(upright[:, i : i + 1], held.shape)
            r.new_state[i, h] = (keep[i : i + 1] * held + key * change[i : i + 1]).astype(
                jnp.bfloat16
            )
        return carry

    scatter = Scatter(
        place,
        r.parts,
        r.plane,
        r.column,
        SUM_CUTS,
        (r.sum_send, r.plane_recv, r.column_recv),
    )
    plan = [heads * i // 16 for i in (0, 5, 9, 13, 16)]

    def fill(i):
        lax.fori_loop(plan[i], plan[i + 1], update, 0)

    ahead = core * (heads * 3 // 16)
    lax.fori_loop(0, ahead, update, 0)
    second.begin()
    lax.fori_loop(ahead, plan[1], update, 0)
    gather.settle()
    settle(r.columns.at[pl.ds(0, pairs - 1)], r.out_sem.at[0], place.partner)
    swaps_settle(("weights",))
    for step in second.relays():
        step()
    fill(1)

    def compute(chunk):
        a, b = 4 * chunk[0], 4 * (chunk[-1] + 1)
        number = (b - a) * count

        r.packed[0:number] = r.rows_two[a:b, :, 0:width].reshape(number, width)
        share = wide(r.rows_two[a:b, :, width:]).reshape(number, LANES)
        lane = lax.rem(lax.broadcasted_iota(jnp.int32, share.shape, 1), HALF)
        share = jnp.sum(jnp.where(lane == place.me // PIECES, share, 0.0), axis=1, keepdims=True)
        for i in range(2):
            for j in range(0, hidden_units, 128):
                rows = r.packed[0:number]
                gated = clamped_unit(
                    jnp.dot(rows, r.wide_in[0, i, :, j : j + 128], preferred_element_type=jnp.float32),
                    jnp.dot(rows, r.wide_in[1, i, :, j : j + 128], preferred_element_type=jnp.float32),
                )
                at = i * hidden_units + j
                r.hidden[0:number, at : at + 128] = gated.astype(jnp.bfloat16)
        for cut, lanes in enumerate(scatter.lanes):
            for j in range(lanes.start, lanes.start + lanes.size, 512):
                weights = r.down[0, :, :, j : j + 512].reshape(2 * hidden_units, 512)
                units = r.hidden[0:number]
                part = jnp.dot(units, weights, preferred_element_type=jnp.float32)
                r.parts[a:b, :, j : j + 512] = (
                    (part * share).astype(jnp.bfloat16).reshape(b - a, count, 512)
                )
            for distance in reversed(chunk):
                scatter.first(distance, cut)

    for number, chunk in enumerate(chunks):
        second.across(number)
        if not number:
            for group in ("wide_in", "down"):
                loaded(group)
                swapped(group)
        compute(chunk)
    fill(2)
    second.settle()
    swaps_settle(("wide_in", "down"))
    for chunk in chunks:
        for cut in range(SUM_CUTS):
            for distance in reversed(chunk):
                scatter.last(distance, cut)
    fill(3)
    for cut in range(SUM_CUTS):
        scatter.collect(cut)
    moe = jnp.concatenate(scatter.values, axis=1)
    r.result[...] = (r.x_second[...] + rms_scale(moe) * r.gains[2]).astype(
        jnp.bfloat16
    )
    scatter.settle()


def store_kernel(result, new_state, result_hbm, state_hbm, sems):
    store = pltpu.make_async_copy(result, result_hbm, sems.at[0])
    store.start()
    for i in range(new_state.shape[0]):
        pltpu.make_async_copy(new_state.at[i], state_hbm.at[i], sems.at[1]).start()
    store.wait()
    pltpu.make_async_copy(new_state, state_hbm, sems.at[1]).wait()


def shards(
    residual_in,
    gain_mix_pre,
    w_query,
    w_key,
    w_value,
    w_outgate,
    w_decay,
    w_beta,
    decay_scale,
    decay_bias,
    head_gain,
    w_out,
    gain_mix_post,
    state_cache,
    gain_ffn_pre,
    routes,
    route_logits,
    w_gate,
    w_up,
    w_down,
    gain_ffn_post,
):
    devices = lax.axis_size("ep")
    layers, pairs = devices // 8, devices // 2
    count, width = residual_in.shape
    heads = w_decay.shape[1]
    own = w_query.shape[1]
    units = w_gate.shape[1]
    rows = 4 * max(1, layers // 2) * count
    if layers > 1:
        rows = max(rows, 4 * (layers - layers // 2) * count)
    inputs = dict(
        x=residual_in,
        gain=gain_mix_pre[None],
        routes=routes.T,
        logits=route_logits.T,
        w_decay=w_decay.T,
        w_beta=w_beta.T,
        scale=decay_scale[None],
        bias=decay_bias[None],
        head_gain=head_gain[None],
        gain_mix=gain_mix_post[None],
        gain_pre=gain_ffn_pre[None],
        gain_post=gain_ffn_post[None],
        query=w_query.T,
        key=w_key.T,
        value=w_value.T,
        outgate=w_outgate.T,
        state=state_cache,
        w_out=w_out,
        gate=w_gate,
        up=w_up,
        down=w_down,
    )
    bf16, f32 = jnp.bfloat16, jnp.float32
    dma = pltpu.SemaphoreType.DMA

    def blocks(number, lanes=width):
        return pltpu.VMEM((number, count, lanes), bf16)

    def per_head():
        return pltpu.VMEM((heads, count, HD), f32)

    def stacked(group):
        first = inputs[GROUPS[group][0]]
        pair = (2,) if group in PAIRED else ()
        many = (len(GROUPS[group]),) if group in PAIRED or len(GROUPS[group]) > 1 else ()
        return pltpu.VMEM(many + pair + first.shape, first.dtype)

    scratch = {group: stacked(group) for group in GROUPS}
    scratch |= dict(
        upright=pltpu.VMEM((width, 8 * own), bf16),
        rows_one=blocks(pairs),
        rows_two=blocks(pairs, width + LANES),
        columns=blocks(pairs, 8 * own),
        joined=blocks(pairs, 8 * own),
        keys=per_head(),
        keep=per_head(),
        beta=per_head(),
        change=per_head(),
        x_second=pltpu.VMEM((count, width), f32),
        hidden=pltpu.VMEM((rows, 2 * units), bf16),
        packed=pltpu.VMEM((rows, width), bf16),
        parts=blocks(pairs),
        plane=blocks(3 * layers),
        column=blocks(layers),
        load_sems=dma((len(GROUPS),)),
        swap_send=dma((len(PAIRED),)),
        swap_recv=dma((len(PAIRED),)),
        one_send=dma((1,)),
        one_column=dma((layers,)),
        one_plane=dma((len(chunks_of(layers)),)),
        two_send=dma((1,)),
        two_column=dma((layers,)),
        two_plane=dma((len(chunks_of(layers)),)),
        out_sem=dma((1,)),
        in_sems=dma((layers,)),
        sum_send=dma((1,)),
        plane_recv=dma((layers, SUM_CUTS)),
        column_recv=dma((SUM_CUTS,)),
    )
    names = [name + "_hbm" for name in INPUTS] + ["result", "new_state"] + list(scratch)
    vmem = pl.BlockSpec(memory_space=pltpu.VMEM)
    hbm = pl.BlockSpec(memory_space=pltpu.HBM)
    held = pl.pallas_call(
        functools.partial(decode_kernel, devices, names),
        out_shape=(
            pltpu.VMEM((count, width), bf16),
            pltpu.VMEM(state_cache.shape, bf16),
        ),
        in_specs=[hbm] * len(INPUTS),
        out_specs=(vmem, vmem),
        scratch_shapes=list(scratch.values()),
        compiler_params=pltpu.CompilerParams(
            collective_id=0, has_side_effects=True, vmem_limit_bytes=VMEM_LIMIT
        ),
    )(*[inputs[name] for name in INPUTS])
    return pl.pallas_call(
        store_kernel,
        out_shape=[jax.ShapeDtypeStruct(a.shape, a.dtype) for a in held],
        in_specs=[vmem] * 2,
        out_specs=[hbm] * 2,
        scratch_shapes=[dma((2,))],
        compiler_params=pltpu.CompilerParams(vmem_limit_bytes=1000 * 1000),
    )(*held)


def solution(mesh):
    in_specs = (
        P("ep", None),
        P(),
        P(None, "ep"),
        P(None, "ep"),
        P(None, "ep"),
        P(None, "ep"),
        P(),
        P(),
        P(),
        P(),
        P(),
        P(),
        P(),
        P("ep", None, None, None),
        P(),
        P("ep", None),
        P("ep", None),
        P(None, "ep"),
        P(None, "ep"),
        P("ep", None),
        P(),
    )
    out_specs = (P("ep", None), P("ep", None, None, None))
    return jax.shard_map(shards, mesh=mesh, in_specs=in_specs, out_specs=out_specs, check_vma=False)
```
